32 devices in a mesh: sp: 4 (over z), dp: 8 (over y, x, core).
Axes of the slice: x: 2, y: 2, z: 4, core: 2. Of those that a mesh axis runs over, the one named last changes fastest.
Arguments:
- queries: bfloat16 [8, 768, 1024], P('dp', 'sp'), may hold values from -6 to 6
- keys: bfloat16 [8, 768, 256], P('dp', 'sp'), may hold values from -6 to 6
- values: bfloat16 [8, 768, 256], P('dp', 'sp'), may hold values from -6 to 6
- query_gain: float32 [64], replicated, may hold values from 0.15 to 7
- key_gain: float32 [64], replicated, may hold values from 0.15 to 7
- out_weight: bfloat16 [1024, 2048], P(None, 'dp'), may hold values from -0.1875 to 0.1875
- out_gain: float32 [2048], replicated, may hold values from 0.1 to 1.9
Outputs:
- output: bfloat16 [8, 768, 2048], P('dp', 'sp')
The draws below stay inside these ranges and needn't reach their ends.
All inputs are finite; a program needn't handle non-finite values.
Results may differ from the reference program's by a relative error of at most 0.0035.
The reference program's roundings to bfloat16 on the way (of `attn_weights` and `attended`) count: a program that leaves them out, or rounds other values in their place, can miss the bound.
Values may be sent and summed in bfloat16 or wider, within the bound.
A program may use at most 64 MiB of HBM per device.

```python
import jax
import jax.numpy as jnp
from jax import lax

D = 2048
QH = 16
KVH = 4
HEAD = 64
GRID_W = 64
SEQ = 768
N_DP = 8


def query_key_pair(key):
    base_key = jax.random.fold_in(key, 11)
    key_a, key_b = jax.random.split(base_key, 2)
    key_draw = jax.random.normal(key_a, (N_DP, SEQ, KVH, HEAD), jnp.float32)
    query_draw = jax.random.normal(key_b, (N_DP, SEQ, QH, HEAD), jnp.float32)
    query_draw = jnp.clip(query_draw, -6.0, 6.0).reshape(N_DP, SEQ, QH * HEAD)
    key_draw = jnp.clip(key_draw, -6.0, 6.0).reshape(N_DP, SEQ, KVH * HEAD)
    return (query_draw, key_draw)


def gain_draw(key, salt):
    spread = 1.0 + 0.18 * jnp.clip(jax.random.normal(jax.random.fold_in(key, salt), (HEAD,), jnp.float32), -4.5, 4.5)
    return spread


def draw_queries(key, part):
    return query_key_pair(key)[0].astype(jnp.bfloat16)


def draw_keys(key, part):
    return query_key_pair(key)[1].astype(jnp.bfloat16)


def draw_query_gain(key, part):
    return gain_draw(key, 21)


def draw_key_gain(key, part):
    return gain_draw(key, 22)


def levels(stream_key, dims, cuts, least, largest):
    def one(dim, parts):
        steps = jax.random.uniform(jax.random.fold_in(jax.random.fold_in(stream_key, 6), dim), (parts,), jnp.float32, least / len(cuts), largest / len(cuts))
        return jnp.repeat(jnp.exp(steps), dims[dim] // parts).reshape((-1,) + (1,) * (len(dims) - dim - 1))

    level = one(*cuts[0])
    for cut in cuts[1:]:
        level = level * one(*cut)
    return level


def bell_draw(own_key, extent, scale, most, cuts=(), held_as=jnp.bfloat16):
    factor_of = levels(own_key, extent, cuts, -0.22, 0.18) if cuts else 1.0
    values = jax.random.normal(own_key, extent, jnp.float32) * scale * factor_of
    return jnp.minimum(jnp.maximum(values, -most), most).astype(held_as)


def setup_inputs(seed: int = 0) -> dict:
    streams_of = jax.random.split(jax.random.key(seed), 8)
    return {
        "queries": draw_queries(jax.random.fold_in(streams_of[7], 71), 0),
        "keys": draw_keys(jax.random.fold_in(streams_of[7], 71), 0),
        "values": bell_draw(streams_of[2], (N_DP, SEQ, KVH * HEAD), 1.0, 6.0, ((0, 8), (1, 4))),
        "query_gain": draw_query_gain(jax.random.fold_in(streams_of[7], 71), 0),
        "key_gain": draw_key_gain(jax.random.fold_in(streams_of[7], 71), 0),
        "out_weight": bell_draw(streams_of[5], (QH * HEAD, D), (QH * HEAD) ** -0.5, 0.1875, ((1, 8),)),
        "out_gain": jnp.clip(1.0 + 0.18 * jax.random.normal(streams_of[6], (D,), jnp.float32), 0.1, 1.9),
    }


EPSILON = 1e-06
ROTARY_BASE = 10000.0

def rotate(vectors, positions, width):
    half_width = width // 2
    frequency = ROTARY_BASE ** (-jnp.arange(0, width, 2, dtype=jnp.float32) / width)
    angles = positions.astype(jnp.float32)[:, None] * frequency[None, :]
    cosines = jnp.cos(angles)[:, None, :]
    sine_table = jnp.sin(angles)[:, None, :]
    first_half = vectors[..., :half_width]
    second_half = vectors[..., half_width:]
    return jnp.concatenate([first_half * cosines - second_half * sine_table, second_half * cosines + first_half * sine_table], axis=-1)

def prepare(vectors, gain_vector, grid_row, grid_col):
    vectors = vectors.astype(jnp.float32)
    vectors = vectors * lax.rsqrt(lax.optimization_barrier(jnp.mean(vectors * vectors, axis=-1, keepdims=True)) + EPSILON) * gain_vector
    half_width = HEAD // 2
    turned = jnp.concatenate([rotate(vectors[..., :half_width], grid_row, half_width), rotate(vectors[..., half_width:], grid_col, half_width)], axis=-1)
    return turned.astype(jnp.bfloat16)

def reference(queries, keys, values, query_gain, key_gain, out_weight, out_gain):
    positions = jnp.arange(SEQ, dtype=jnp.int32)
    grid_row = positions // GRID_W
    grid_col = positions % GRID_W
    group_size = QH // KVH
    score_scale = HEAD ** (-0.5)

    def one_sequence(operands):
        query_seq, key_seq, value_seq = operands
        query_rot = prepare(query_seq.reshape(SEQ, QH, HEAD), query_gain, grid_row, grid_col)
        key_rot = prepare(key_seq.reshape(SEQ, KVH, HEAD), key_gain, grid_row, grid_col)
        value_heads = value_seq.reshape(SEQ, KVH, HEAD)

        def one_head(head_index):
            query_head = lax.dynamic_index_in_dim(query_rot, head_index, 1, keepdims=False)
            key_head = lax.dynamic_index_in_dim(key_rot, head_index // group_size, 1, keepdims=False)
            value_head = lax.dynamic_index_in_dim(value_heads, head_index // group_size, 1, keepdims=False)
            scores = jnp.dot(query_head, key_head.T, preferred_element_type=jnp.float32) * score_scale
            row_max = lax.optimization_barrier(jnp.max(scores, axis=-1, keepdims=True))
            exponent = jnp.exp(scores - row_max)
            attn_weights = (exponent / lax.optimization_barrier(jnp.sum(exponent, axis=-1, keepdims=True))).astype(jnp.bfloat16)
            return jnp.dot(attn_weights, value_head, preferred_element_type=jnp.float32).astype(jnp.bfloat16)
        per_head = lax.map(one_head, jnp.arange(QH, dtype=jnp.int32))
        attended = per_head.transpose(1, 0, 2).reshape(SEQ, QH * HEAD)
        projected = jnp.dot(attended, out_weight, preferred_element_type=jnp.float32)
        projected = projected * lax.rsqrt(lax.optimization_barrier(jnp.mean(projected * projected, axis=-1, keepdims=True)) + EPSILON) * out_gain
        return projected.astype(jnp.bfloat16)
    return lax.map(one_sequence, (queries, keys, values))
```

```python
import functools

import jax
import jax.numpy as jnp
import numpy as np
from jax import lax
from jax.experimental import pallas as pl
from jax.experimental.pallas import tpu as pltpu
from jax.sharding import PartitionSpec as P

QH = 16
KVH = 4
HEAD = 64
GRID_W = 64
GROUP = QH // KVH
BLOCK = GROUP * HEAD


EPSILON = 1e-06
ROTARY_BASE = 10000.0

F32 = jnp.float32
BF16 = jnp.bfloat16


def rotate(vectors, positions, width):
    half_width = width // 2
    frequency = ROTARY_BASE ** (-jnp.arange(0, width, 2, dtype=jnp.float32) / width)
    angles = positions.astype(jnp.float32)[:, None] * frequency[None, :]
    cosines = jnp.cos(angles)[:, None, :]
    sine_table = jnp.sin(angles)[:, None, :]
    first_half = vectors[..., :half_width]
    second_half = vectors[..., half_width:]
    return jnp.concatenate(
        [
            first_half * cosines - second_half * sine_table,
            second_half * cosines + first_half * sine_table,
        ],
        axis=-1,
    )


def prepare(vectors, gain_vector, grid_row, grid_col):
    vectors = vectors.astype(jnp.float32)
    vectors = (
        vectors
        * lax.rsqrt(jnp.mean(vectors * vectors, axis=-1, keepdims=True) + EPSILON)
        * gain_vector
    )
    half_width = HEAD // 2
    turned = jnp.concatenate(
        [
            rotate(vectors[..., :half_width], grid_row, half_width),
            rotate(vectors[..., half_width:], grid_col, half_width),
        ],
        axis=-1,
    )
    return turned.astype(jnp.bfloat16)


def softmax_rows(scores):
    row_max = jnp.max(scores, axis=-1, keepdims=True)
    exponent = jnp.exp(scores - row_max)
    return exponent / jnp.sum(exponent, axis=-1, keepdims=True)


def per_device_general(queries, keys, values, query_gain, key_gain, out_weight, out_gain):
    sp_count = lax.axis_size("sp")
    tokens_here = queries.shape[1]
    seq_len = tokens_here * sp_count
    score_scale = HEAD ** (-0.5)
    offset = lax.axis_index("sp") * tokens_here
    positions = offset + jnp.arange(tokens_here, dtype=jnp.int32)
    grid_row = positions // GRID_W
    grid_col = positions % GRID_W
    query_rot = prepare(queries[0].reshape(tokens_here, QH, HEAD), query_gain, grid_row, grid_col)
    key_rot = prepare(keys[0].reshape(tokens_here, KVH, HEAD), key_gain, grid_row, grid_col)
    value_heads = values[0].reshape(tokens_here, KVH, HEAD)
    kv_pairs = jnp.concatenate([key_rot, value_heads], axis=2)
    all_pairs = lax.all_gather(
        kv_pairs.reshape(tokens_here, KVH * 2 * HEAD), "sp", axis=0, tiled=True
    )
    all_pairs = all_pairs.reshape(seq_len, KVH, 2, HEAD)
    key_all = all_pairs[:, :, 0].transpose(1, 0, 2)
    value_all = all_pairs[:, :, 1].transpose(1, 0, 2)
    query_groups = query_rot.reshape(tokens_here, KVH, QH // KVH, HEAD).transpose(1, 0, 2, 3)

    def attend_group(operands):
        query_group, key_head, value_head = operands
        scores = (
            jnp.einsum("qgd,kd->gqk", query_group, key_head, preferred_element_type=jnp.float32)
            * score_scale
        )
        attn_weights = softmax_rows(scores).astype(jnp.bfloat16)
        return jnp.einsum(
            "gqk,kd->qgd", attn_weights, value_head, preferred_element_type=jnp.float32
        ).astype(jnp.bfloat16)

    results = lax.map(attend_group, (query_groups, key_all, value_all))
    attended = results.transpose(1, 0, 2, 3).reshape(tokens_here, QH * HEAD)
    projected = jnp.dot(
        attended,
        lax.all_gather(out_weight, "dp", axis=1, tiled=True),
        preferred_element_type=jnp.float32,
    )
    normed = (
        projected
        * lax.rsqrt(jnp.mean(projected * projected, axis=-1, keepdims=True) + EPSILON)
        * out_gain
    )
    return normed.astype(jnp.bfloat16)[None]


def position_tables(seq_len):
    width = HEAD // 2
    frequency = np.float32(ROTARY_BASE) ** (
        -np.arange(0, width, 2, dtype=np.float32) / np.float32(width)
    )
    position = np.arange(seq_len)
    parts = []
    for coordinate in (position // GRID_W, position % GRID_W):
        angles = coordinate.astype(np.float32)[:, None] * frequency[None, :]
        parts += [angles, angles]
    angles = np.concatenate(parts * 2, axis=1).astype(np.float64)
    return np.stack([np.cos(angles), np.sin(angles)]).astype(np.float32)


def dot(a, b):
    return jnp.dot(a, b, preferred_element_type=F32)


def kernel(
    sp, dp,
    q_ref, k_ref, v_ref, qg_ref, kg_ref, w_ref, og_ref, table_ref,
    out_ref,
    q_raw, q_rot, k_all, v_all, k_rot, tables, w_all, gains,
    swap_mat, ones_mat, expo, peak, total, att, proj,
    local_sem, kv_send, kv_recv, w_send, w_recv,
):
    tokens = q_raw.shape[0]
    depth = w_ref.shape[0]
    half = depth // 2
    me = lax.axis_index("sp")
    here = lax.axis_index("dp")
    mate = here + 1 - 2 * (here % 2)
    flip_x = 2 - 4 * ((here // 2) % 2)
    flip_y = 4 - 8 * ((here // 4) % 2)
    dev_x = here + flip_x
    dev_y = here + flip_y
    dev_d = here + flip_x + flip_y

    barrier = pltpu.get_barrier_semaphore()
    has_left = me > 0
    has_right = me < sp - 1

    for other in (mate, dev_x, dev_y):
        pl.semaphore_signal(barrier, inc=1, device_id={"dp": other})

    @pl.when(has_left)
    def _():
        pl.semaphore_signal(barrier, inc=1, device_id={"sp": me - 1})

    @pl.when(has_right)
    def _():
        pl.semaphore_signal(barrier, inc=1, device_id={"sp": me + 1})

    locals_ = [
        pltpu.make_async_copy(q_ref, q_raw, local_sem.at[0]),
        pltpu.make_async_copy(table_ref, tables, local_sem.at[1]),
        pltpu.make_async_copy(k_ref, k_all.at[pl.ds(me * tokens, tokens)], local_sem.at[2]),
        pltpu.make_async_copy(v_ref, v_all.at[pl.ds(me * tokens, tokens)], local_sem.at[3]),
        pltpu.make_async_copy(w_ref, w_all.at[here], local_sem.at[4]),
    ]
    for copy in locals_:
        copy.start()

    pl.semaphore_wait(barrier, 3 + jnp.minimum(me, 1) + jnp.minimum(sp - 1 - me, 1))

    def kv_copies(way, step):
        block = me - step if way == 0 else me + step
        target = me + 1 if way == 0 else me - 1
        rows = pl.ds(block * tokens, tokens)
        copies = []
        for i, (own, every) in enumerate(((k_ref, k_all), (v_ref, v_all))):
            copies.append(
                pltpu.make_async_remote_copy(
                    src_ref=own if step == 0 else every.at[rows],
                    dst_ref=every.at[rows],
                    send_sem=kv_send.at[way, step, i],
                    recv_sem=kv_recv.at[way, step, i],
                    device_id={"sp": target},
                )
            )
        return copies

    def kv_sends(way, step):
        if way == 0:
            return jnp.logical_and(has_right, me - step >= 0)
        return jnp.logical_and(has_left, me + step < sp)

    def kv_start(step):
        for way in (0, 1):
            @pl.when(kv_sends(way, step))
            def _(way=way):
                for copy in kv_copies(way, step):
                    copy.start()

    def kv_wait_recv(step):
        for way in (0, 1):
            source = me - 1 - step if way == 0 else me + 1 + step
            arrives = source >= 0 if way == 0 else source < sp

            @pl.when(arrives)
            def _(way=way, source=source):
                rows = pl.ds(source * tokens, tokens)
                for i, every in enumerate((k_all, v_all)):
                    pltpu.make_async_remote_copy(
                        src_ref=every.at[rows],
                        dst_ref=every.at[rows],
                        send_sem=kv_send.at[way, step, i],
                        recv_sem=kv_recv.at[way, step, i],
                        device_id={"sp": me},
                    ).wait_recv()

    kv_start(0)

    top, bottom, whole = (0, half), (half, half), (0, depth)

    def w_copy(index, shard, rows, target, own=False):
        window = pl.ds(rows[0], rows[1])
        return pltpu.make_async_remote_copy(
            src_ref=w_ref.at[window] if own else w_all.at[shard, window],
            dst_ref=w_all.at[shard, window],
            send_sem=w_send.at[index],
            recv_sem=w_recv.at[index],
            device_id={"dp": target},
        )

    def w_wait(index, shard, rows):
        w_copy(index, shard, rows, mate).wait_recv()

    sent = [
        w_copy(0, here, bottom, dev_x, own=True),
        w_copy(2, here, top, dev_y, own=True),
        w_copy(1, here, top, dev_x, own=True),
        w_copy(3, here, bottom, dev_y, own=True),
        w_copy(6, here, whole, mate, own=True),
    ]
    for copy in sent:
        copy.start()

    def w_forward(index, shard, rows, target):
        copy = w_copy(index, shard, rows, target)
        copy.start()
        sent.append(copy)

    row_id = lax.broadcasted_iota(jnp.int32, (BLOCK, BLOCK), 0)
    col_id = lax.broadcasted_iota(jnp.int32, (BLOCK, BLOCK), 1)
    quarter = HEAD // 4
    second = (col_id & (HEAD // 2 - 1)) >= quarter
    partner_col = jnp.where(second, col_id - quarter, col_id + quarter)
    hit = row_id == partner_col
    swap_mat[...] = jnp.where(hit, jnp.where(second, 1.0, -1.0), 0.0).astype(BF16)
    ones_mat[...] = jnp.where((row_id // HEAD) == (col_id // HEAD), 1.0, 0.0).astype(BF16)
    spread = jnp.where(
        row_id[:HEAD] == (col_id[:HEAD] & (HEAD - 1)), 1.0, 0.0
    ).astype(BF16)
    spread_swapped = jnp.where(
        row_id[:HEAD] == (partner_col[:HEAD] & (HEAD - 1)), 1.0, 0.0
    ).astype(BF16)
    for i, gain_ref in enumerate((qg_ref, kg_ref)):
        gain = jnp.broadcast_to(gain_ref[...], (16, HEAD))
        first = gain.astype(BF16)
        rest = gain - first.astype(F32)
        mid = rest.astype(BF16)
        low = (rest - mid.astype(F32)).astype(BF16)
        for j, matrix in enumerate((spread, spread_swapped)):
            gains[2 * i + j] = (dot(first, matrix) + dot(mid, matrix)) + dot(low, matrix)

    lane_head = lax.broadcasted_iota(jnp.int32, (1, BLOCK), 1) // HEAD
    masks = [jnp.where(lane_head == p, 1.0, 0.0) for p in range(GROUP)]

    def turned(x, rows, which, scale):
        xf = x.astype(F32)
        square = xf * xf
        high = square.astype(BF16)
        low = (square - high.astype(F32)).astype(BF16)
        ones = ones_mat[...]
        mean = (dot(high, ones) + dot(low, ones)) * (1.0 / HEAD)
        inverse = lax.rsqrt(mean + EPSILON) * scale
        swapped = dot(x, swap_mat[...])
        cosines = tables[0, rows, :]
        sines = tables[1, rows, :]
        cosines = jnp.concatenate([cosines, cosines], axis=1) * gains[2 * which, 0:1, :]
        sines = jnp.concatenate([sines, sines], axis=1) * gains[2 * which + 1, 0:1, :]
        return ((xf * cosines + swapped * sines) * inverse).astype(BF16)

    locals_[0].wait()
    locals_[1].wait()
    own_rows = pl.ds(pl.multiple_of(me * tokens, 64), tokens)
    for b in range(KVH):
        columns = slice(b * BLOCK, (b + 1) * BLOCK)
        q_rot[:, columns] = turned(q_raw[:, columns], own_rows, 0, HEAD ** (-0.5))

    pairs = sp // 2
    mine = me // 2

    def attend(turn):
        span = 2 * tokens
        pair = lax.rem(mine + turn, pairs)
        rows = pl.ds(pl.multiple_of(pair * span, 128), span)
        k_rot[...] = turned(k_all[rows, :], rows, 1, 1.0)
        before = [pl.ds(pl.multiple_of(lax.rem(mine + t, pairs) * span, 128), span) for t in range(turn)]

        def one(b, carry):
            columns = pl.ds(pl.multiple_of(b * BLOCK, BLOCK), BLOCK)
            pick = jnp.where(row_id == b * HEAD + (col_id & (HEAD - 1)), 1.0, 0.0).astype(BF16)
            key = dot(k_rot[...], pick).astype(BF16)
            query = q_rot[:, columns]
            if turn == pairs - 1:
                value = dot(v_all[rows, :], pick).astype(BF16)
                olds = [dot(v_all[r, :], pick).astype(BF16) for r in before]
            out = 0.0
            for p in range(GROUP):
                mask = masks[p]
                head = b * GROUP + p
                scores = lax.dot_general(
                    query * mask.astype(BF16), key, (((1,), (1,)), ((), ())),
                    preferred_element_type=F32,
                )
                high = jnp.max(scores, axis=1, keepdims=True)
                if turn < pairs - 1:
                    weights = jnp.exp(scores - high)
                    expo[turn, head] = weights
                    peak[turn, head] = high
                    total[turn, head] = jnp.sum(weights, axis=1, keepdims=True)
                    continue
                for t in range(turn):
                    high = jnp.maximum(high, peak[t, head])
                weights = jnp.exp(scores - high)
                norm = jnp.sum(weights, axis=1, keepdims=True)
                keeps = [jnp.exp(peak[t, head] - high) for t in range(turn)]
                for t in range(turn):
                    norm = norm + total[t, head] * keeps[t]
                inverse = 1.0 / norm
                product = dot((weights * inverse).astype(BF16), value)
                for t in range(turn):
                    old = expo[t, head] * (keeps[t] * inverse)
                    product = product + dot(old.astype(BF16), olds[t])
                out = out + product * mask
            if turn == pairs - 1:
                att[:, columns] = out.astype(BF16)
            return carry

        lax.fori_loop(0, KVH, one, 0)

    locals_[2].wait()
    locals_[3].wait()

    kv_wait_recv(0)
    if sp > 2:
        kv_start(1)

    w_wait(0, dev_x, bottom)
    w_forward(5, dev_x, bottom, dev_y)
    w_wait(2, dev_y, top)
    w_forward(4, dev_y, top, dev_x)
    w_forward(7, dev_x, bottom, mate)
    w_forward(9, dev_y, top, mate)

    attend(0)
    for step in range(1, sp - 1):
        kv_wait_recv(step)
        if step < sp - 2:
            kv_start(step + 1)
    w_wait(1, dev_x, top)
    w_forward(8, dev_x, top, mate)
    w_wait(3, dev_y, bottom)
    w_forward(10, dev_y, bottom, mate)
    for turn in range(1, pairs):
        attend(turn)

    columns_each = w_ref.shape[1]

    def project(shard, squares):
        columns = pl.ds(pl.multiple_of(shard * columns_each, columns_each), columns_each)
        result = dot(att[...], w_all[shard])
        proj[:, columns] = result
        return squares + jnp.sum(result * result, axis=1, keepdims=True)

    mate_x, mate_y, mate_d = mate + flip_x, mate + flip_y, mate + flip_x + flip_y
    locals_[4].wait()
    squares = project(here, jnp.zeros((tokens, 1), F32))
    w_wait(6, mate, whole)
    squares = project(mate, squares)
    squares = project(dev_x, squares)
    squares = project(dev_y, squares)
    w_wait(7, mate_x, bottom)
    w_wait(8, mate_x, top)
    squares = project(mate_x, squares)
    w_wait(9, mate_y, top)
    w_wait(10, mate_y, bottom)
    squares = project(mate_y, squares)
    w_wait(4, dev_d, top)
    w_forward(11, dev_d, top, mate)
    w_wait(5, dev_d, bottom)
    w_forward(12, dev_d, bottom, mate)
    squares = project(dev_d, squares)
    w_wait(11, mate_d, top)
    w_wait(12, mate_d, bottom)
    squares = project(mate_d, squares)

    inverse = lax.rsqrt(squares * (1.0 / (columns_each * dp)) + EPSILON)
    for j in range(dp):
        columns = slice(j * columns_each, (j + 1) * columns_each)
        out_ref[:, columns] = (proj[:, columns] * inverse * og_ref[:, columns]).astype(BF16)

    for copy in sent:
        copy.wait_send()
    for step in range(sp - 1):
        for way in (0, 1):
            @pl.when(kv_sends(way, step))
            def _(way=way, step=step):
                for copy in kv_copies(way, step):
                    copy.wait_send()


def per_device_fused(sp, dp, queries, keys, values, query_gain, key_gain, out_weight, out_gain):
    tokens = queries.shape[1]
    depth, columns = out_weight.shape
    hidden = queries.shape[2]
    kv_width = keys.shape[2]
    seq_len = tokens * sp
    hbm_spec = pl.BlockSpec(memory_space=pltpu.HBM)
    vmem_spec = pl.BlockSpec(memory_space=pltpu.VMEM)
    result = pl.pallas_call(
        functools.partial(kernel, sp, dp),
        out_shape=jax.ShapeDtypeStruct((tokens, columns * dp), BF16),
        in_specs=[hbm_spec] * 3 + [vmem_spec] * 2 + [hbm_spec, vmem_spec, hbm_spec],
        out_specs=vmem_spec,
        scratch_shapes=[
            pltpu.VMEM((tokens, hidden), BF16),
            pltpu.VMEM((tokens, hidden), BF16),
            pltpu.VMEM((seq_len, kv_width), BF16),
            pltpu.VMEM((seq_len, kv_width), BF16),
            pltpu.VMEM((2 * tokens, kv_width), BF16),
            pltpu.VMEM((2, seq_len, 2 * HEAD), F32),
            pltpu.VMEM((dp, depth, columns), BF16),
            pltpu.VMEM((4, 16, BLOCK), F32),
            pltpu.VMEM((BLOCK, BLOCK), BF16),
            pltpu.VMEM((BLOCK, BLOCK), BF16),
            pltpu.VMEM((max(sp // 2 - 1, 1), QH, tokens, 2 * tokens), F32),
            pltpu.VMEM((max(sp // 2 - 1, 1), QH, tokens, 1), F32),
            pltpu.VMEM((max(sp // 2 - 1, 1), QH, tokens, 1), F32),
            pltpu.VMEM((tokens, hidden), BF16),
            pltpu.VMEM((tokens, columns * dp), F32),
            pltpu.SemaphoreType.DMA((5,)),
            pltpu.SemaphoreType.DMA((2, sp - 1, 2)),
            pltpu.SemaphoreType.DMA((2, sp - 1, 2)),
            pltpu.SemaphoreType.DMA((13,)),
            pltpu.SemaphoreType.DMA((13,)),
        ],
        compiler_params=pltpu.CompilerParams(
            collective_id=0, has_side_effects=True, vmem_limit_bytes=48 * 1024 * 1024
        ),
    )(
        queries[0], keys[0], values[0], query_gain[None], key_gain[None],
        out_weight, out_gain[None], jnp.asarray(position_tables(seq_len)),
    )
    return result[None]


def solution(mesh):
    sp, dp = mesh.shape["sp"], mesh.shape["dp"]
    if dp == 8 and sp >= 2 and sp % 2 == 0 and sp <= 4:
        body = functools.partial(per_device_fused, sp, dp)
    else:
        body = per_device_general
    return jax.shard_map(
        body,
        mesh=mesh,
        in_specs=(
            P("dp", "sp", None),
            P("dp", "sp", None),
            P("dp", "sp", None),
            P(),
            P(),
            P(None, "dp"),
            P(),
        ),
        out_specs=P("dp", "sp", None),
        check_vma=False,
    )
```

```python
import functools

import jax
import jax.numpy as jnp
import numpy as np
from jax import lax
from jax.experimental import pallas as pl
from jax.experimental.pallas import tpu as pltpu
from jax.sharding import PartitionSpec as P

QH = 16
KVH = 4
HEAD = 64
GRID_W = 64
GROUP = QH // KVH
BLOCK = GROUP * HEAD


EPSILON = 1e-06
ROTARY_BASE = 10000.0

F32 = jnp.float32
BF16 = jnp.bfloat16


def rotate(vectors, positions, width):
    half_width = width // 2
    frequency = ROTARY_BASE ** (-jnp.arange(0, width, 2, dtype=jnp.float32) / width)
    angles = positions.astype(jnp.float32)[:, None] * frequency[None, :]
    cosines = jnp.cos(angles)[:, None, :]
    sine_table = jnp.sin(angles)[:, None, :]
    first_half = vectors[..., :half_width]
    second_half = vectors[..., half_width:]
    return jnp.concatenate(
        [
            first_half * cosines - second_half * sine_table,
            second_half * cosines + first_half * sine_table,
        ],
        axis=-1,
    )


def prepare(vectors, gain_vector, grid_row, grid_col):
    vectors = vectors.astype(jnp.float32)
    vectors = (
        vectors
        * lax.rsqrt(jnp.mean(vectors * vectors, axis=-1, keepdims=True) + EPSILON)
        * gain_vector
    )
    half_width = HEAD // 2
    turned = jnp.concatenate(
        [
            rotate(vectors[..., :half_width], grid_row, half_width),
            rotate(vectors[..., half_width:], grid_col, half_width),
        ],
        axis=-1,
    )
    return turned.astype(jnp.bfloat16)


def softmax_rows(scores):
    row_max = jnp.max(scores, axis=-1, keepdims=True)
    exponent = jnp.exp(scores - row_max)
    return exponent / jnp.sum(exponent, axis=-1, keepdims=True)


def per_device_general(queries, keys, values, query_gain, key_gain, out_weight, out_gain):
    sp_count = lax.axis_size("sp")
    tokens_here = queries.shape[1]
    seq_len = tokens_here * sp_count
    score_scale = HEAD ** (-0.5)
    offset = lax.axis_index("sp") * tokens_here
    positions = offset + jnp.arange(tokens_here, dtype=jnp.int32)
    grid_row = positions // GRID_W
    grid_col = positions % GRID_W
    query_rot = prepare(queries[0].reshape(tokens_here, QH, HEAD), query_gain, grid_row, grid_col)
    key_rot = prepare(keys[0].reshape(tokens_here, KVH, HEAD), key_gain, grid_row, grid_col)
    value_heads = values[0].reshape(tokens_here, KVH, HEAD)
    kv_pairs = jnp.concatenate([key_rot, value_heads], axis=2)
    all_pairs = lax.all_gather(
        kv_pairs.reshape(tokens_here, KVH * 2 * HEAD), "sp", axis=0, tiled=True
    )
    all_pairs = all_pairs.reshape(seq_len, KVH, 2, HEAD)
    key_all = all_pairs[:, :, 0].transpose(1, 0, 2)
    value_all = all_pairs[:, :, 1].transpose(1, 0, 2)
    query_groups = query_rot.reshape(tokens_here, KVH, QH // KVH, HEAD).transpose(1, 0, 2, 3)

    def attend_group(operands):
        query_group, key_head, value_head = operands
        scores = (
            jnp.einsum("qgd,kd->gqk", query_group, key_head, preferred_element_type=jnp.float32)
            * score_scale
        )
        attn_weights = softmax_rows(scores).astype(jnp.bfloat16)
        return jnp.einsum(
            "gqk,kd->qgd", attn_weights, value_head, preferred_element_type=jnp.float32
        ).astype(jnp.bfloat16)

    results = lax.map(attend_group, (query_groups, key_all, value_all))
    attended = results.transpose(1, 0, 2, 3).reshape(tokens_here, QH * HEAD)
    projected = jnp.dot(
        attended,
        lax.all_gather(out_weight, "dp", axis=1, tiled=True),
        preferred_element_type=jnp.float32,
    )
    normed = (
        projected
        * lax.rsqrt(jnp.mean(projected * projected, axis=-1, keepdims=True) + EPSILON)
        * out_gain
    )
    return normed.astype(jnp.bfloat16)[None]


def position_tables(seq_len):
    width = HEAD // 2
    frequency = np.float32(ROTARY_BASE) ** (
        -np.arange(0, width, 2, dtype=np.float32) / np.float32(width)
    )
    position = np.arange(seq_len)
    parts = []
    for coordinate in (position // GRID_W, position % GRID_W):
        angles = coordinate.astype(np.float32)[:, None] * frequency[None, :]
        parts += [angles, angles]
    angles = np.concatenate(parts * 2, axis=1).astype(np.float64)
    return np.stack([np.cos(angles), np.sin(angles)]).astype(np.float32)


def dot(a, b):
    return jnp.dot(a, b, preferred_element_type=F32)


def cross(a, b):
    return lax.dot_general(a, b, (((1,), (1,)), ((), ())), preferred_element_type=F32)


def kernel(
    sp, dp,
    q_ref, k_ref, v_ref, qg_ref, kg_ref, w_ref, og_ref, table_ref,
    out_ref,
    q_raw, q_rot, k_all, v_all, k_rot, tables, w_all, gains,
    swap_mat, ones_mat, place_mat, back_mat, v_turned,
    expo, peak, total, att, proj,
    local_sem, kv_send, kv_recv, w_send, w_recv,
):
    tokens = q_raw.shape[0]
    depth = w_ref.shape[0]
    half = depth // 2
    me = lax.axis_index("sp")
    here = lax.axis_index("dp")
    mate = here + 1 - 2 * (here % 2)
    flip_x = 2 - 4 * ((here // 2) % 2)
    flip_y = 4 - 8 * ((here // 4) % 2)
    dev_x = here + flip_x
    dev_y = here + flip_y
    dev_d = here + flip_x + flip_y

    barrier = pltpu.get_barrier_semaphore()
    has_left = me > 0
    has_right = me < sp - 1

    for other in (mate, dev_x, dev_y):
        pl.semaphore_signal(barrier, inc=1, device_id={"dp": other})

    @pl.when(has_left)
    def _():
        pl.semaphore_signal(barrier, inc=1, device_id={"sp": me - 1})

    @pl.when(has_right)
    def _():
        pl.semaphore_signal(barrier, inc=1, device_id={"sp": me + 1})

    locals_ = [
        pltpu.make_async_copy(q_ref, q_raw, local_sem.at[0]),
        pltpu.make_async_copy(table_ref, tables, local_sem.at[1]),
        pltpu.make_async_copy(k_ref, k_all.at[pl.ds(me * tokens, tokens)], local_sem.at[2]),
        pltpu.make_async_copy(v_ref, v_all.at[pl.ds(me * tokens, tokens)], local_sem.at[3]),
        pltpu.make_async_copy(w_ref, w_all.at[here], local_sem.at[4]),
    ]
    for copy in locals_:
        copy.start()

    pl.semaphore_wait(barrier, 3 + jnp.minimum(me, 1) + jnp.minimum(sp - 1 - me, 1))

    def kv_copies(way, step):
        block = me - step if way == 0 else me + step
        target = me + 1 if way == 0 else me - 1
        rows = pl.ds(block * tokens, tokens)
        copies = []
        for i, (own, every) in enumerate(((k_ref, k_all), (v_ref, v_all))):
            copies.append(
                pltpu.make_async_remote_copy(
                    src_ref=own if step == 0 else every.at[rows],
                    dst_ref=every.at[rows],
                    send_sem=kv_send.at[way, step, i],
                    recv_sem=kv_recv.at[way, step, i],
                    device_id={"sp": target},
                )
            )
        return copies

    def kv_sends(way, step):
        if way == 0:
            return jnp.logical_and(has_right, me - step >= 0)
        return jnp.logical_and(has_left, me + step < sp)

    def kv_start(step):
        for way in (0, 1):
            @pl.when(kv_sends(way, step))
            def _(way=way):
                for copy in kv_copies(way, step):
                    copy.start()

    def kv_wait_recv(step):
        for way in (0, 1):
            source = me - 1 - step if way == 0 else me + 1 + step
            arrives = source >= 0 if way == 0 else source < sp

            @pl.when(arrives)
            def _(way=way, source=source):
                rows = pl.ds(source * tokens, tokens)
                for i, every in enumerate((k_all, v_all)):
                    pltpu.make_async_remote_copy(
                        src_ref=every.at[rows],
                        dst_ref=every.at[rows],
                        send_sem=kv_send.at[way, step, i],
                        recv_sem=kv_recv.at[way, step, i],
                        device_id={"sp": me},
                    ).wait_recv()

    kv_start(0)

    top, bottom, whole = (0, half), (half, half), (0, depth)

    def w_copy(index, shard, rows, target, own=False):
        window = pl.ds(rows[0], rows[1])
        return pltpu.make_async_remote_copy(
            src_ref=w_ref.at[window] if own else w_all.at[shard, window],
            dst_ref=w_all.at[shard, window],
            send_sem=w_send.at[index],
            recv_sem=w_recv.at[index],
            device_id={"dp": target},
        )

    def w_wait(index, shard, rows):
        w_copy(index, shard, rows, mate).wait_recv()

    sent = [
        w_copy(0, here, bottom, dev_x, own=True),
        w_copy(2, here, top, dev_y, own=True),
        w_copy(1, here, top, dev_x, own=True),
        w_copy(3, here, bottom, dev_y, own=True),
        w_copy(6, here, whole, mate, own=True),
    ]
    for copy in sent:
        copy.start()

    def w_forward(index, shard, rows, target):
        copy = w_copy(index, shard, rows, target)
        copy.start()
        sent.append(copy)

    row_id = lax.broadcasted_iota(jnp.int32, (BLOCK, BLOCK), 0)
    col_id = lax.broadcasted_iota(jnp.int32, (BLOCK, BLOCK), 1)
    quarter = HEAD // 4
    second = (col_id & (HEAD // 2 - 1)) >= quarter
    partner_col = jnp.where(second, col_id - quarter, col_id + quarter)
    hit = row_id == partner_col
    swap_mat[...] = jnp.where(hit, jnp.where(second, 1.0, -1.0), 0.0).astype(BF16)
    ones_mat[...] = jnp.where((row_id // HEAD) == (col_id // HEAD), 1.0, 0.0).astype(BF16)
    spread = jnp.where(
        row_id[:HEAD] == (col_id[:HEAD] & (HEAD - 1)), 1.0, 0.0
    ).astype(BF16)
    spread_swapped = jnp.where(
        row_id[:HEAD] == (partner_col[:HEAD] & (HEAD - 1)), 1.0, 0.0
    ).astype(BF16)
    for i, gain_ref in enumerate((qg_ref, kg_ref)):
        gain = jnp.broadcast_to(gain_ref[...], (16, HEAD))
        first = gain.astype(BF16)
        rest = gain - first.astype(F32)
        mid = rest.astype(BF16)
        low = (rest - mid.astype(F32)).astype(BF16)
        for j, matrix in enumerate((spread, spread_swapped)):
            gains[2 * i + j] = (dot(first, matrix) + dot(mid, matrix)) + dot(low, matrix)

    lane_head = lax.broadcasted_iota(jnp.int32, (1, BLOCK), 1) // HEAD
    masks = [jnp.where(lane_head == p, 1.0, 0.0) for p in range(GROUP)]

    def turned(x, rows, which, scale):
        xf = x.astype(F32)
        square = xf * xf
        high = square.astype(BF16)
        low = (square - high.astype(F32)).astype(BF16)
        ones = ones_mat[...]
        mean = (dot(high, ones) + dot(low, ones)) * (1.0 / HEAD)
        inverse = lax.rsqrt(mean + EPSILON) * scale
        swapped = dot(x, swap_mat[...])
        cosines = tables[0, rows, :]
        sines = tables[1, rows, :]
        cosines = jnp.concatenate([cosines, cosines], axis=1) * gains[2 * which, 0:1, :]
        sines = jnp.concatenate([sines, sines], axis=1) * gains[2 * which + 1, 0:1, :]
        return ((xf * cosines + swapped * sines) * inverse).astype(BF16)

    locals_[0].wait()
    locals_[1].wait()
    own_rows = pl.ds(pl.multiple_of(me * tokens, 64), tokens)
    for b in range(KVH):
        columns = slice(b * BLOCK, (b + 1) * BLOCK)
        q_rot[:, columns] = turned(q_raw[:, columns], own_rows, 0, HEAD ** (-0.5))

    pairs = sp // 2
    mine = me // 2

    eye = jnp.where(row_id == col_id, 1.0, 0.0).astype(BF16)
    wide = GROUP * tokens
    lane = lax.broadcasted_iota(jnp.int32, (BLOCK, wide), 1)
    line = lax.broadcasted_iota(jnp.int32, (BLOCK, wide), 0) // HEAD * tokens
    inside = jnp.logical_and(lane >= line, lane < line + tokens)
    place_mat[...] = jnp.where(inside, 1.0, 0.0).astype(BF16)
    lane = lax.broadcasted_iota(jnp.int32, (tokens, wide), 1)
    line = lax.broadcasted_iota(jnp.int32, (tokens, wide), 0)
    hit = lane == line
    for p in range(1, GROUP):
        hit = jnp.logical_or(hit, lane == line + p * tokens)
    back_mat[...] = jnp.where(hit, 1.0, 0.0).astype(BF16)

    def attend(turn):
        span = 2 * tokens
        pair = lax.rem(mine + turn, pairs)
        rows = pl.ds(pl.multiple_of(pair * span, 128), span)
        k_rot[...] = turned(k_all[rows, :], rows, 1, 1.0)
        v_turned[turn] = cross(eye, v_all[rows, :]).astype(BF16)

        def one(b, carry):
            columns = pl.ds(pl.multiple_of(b * BLOCK, BLOCK), BLOCK)
            value_rows = pl.ds(pl.multiple_of(b * HEAD, HEAD), HEAD)
            pick = jnp.where(row_id == b * HEAD + (col_id & (HEAD - 1)), 1.0, 0.0).astype(BF16)
            key = dot(k_rot[...], pick).astype(BF16)
            query = q_rot[:, columns]
            query = jnp.concatenate([query * mask.astype(BF16) for mask in masks], axis=0)
            scores = cross(key, query)
            high = jnp.max(scores, axis=0, keepdims=True)
            if turn < pairs - 1:
                weights = jnp.exp(scores - high)
                expo[turn, b] = weights
                peak[turn, b] = high
                total[turn, b] = jnp.sum(weights, axis=0, keepdims=True)
                return carry
            for t in range(turn):
                high = jnp.maximum(high, peak[t, b])
            weights = jnp.exp(scores - high)
            norm = jnp.sum(weights, axis=0, keepdims=True)
            keeps = [jnp.exp(peak[t, b] - high) for t in range(turn)]
            for t in range(turn):
                norm = norm + total[t, b] * keeps[t]
            inverse = 1.0 / norm
            product = dot(v_turned[turn, value_rows, :], (weights * inverse).astype(BF16))
            for t in range(turn):
                old = expo[t, b] * (keeps[t] * inverse)
                product = product + dot(v_turned[t, value_rows, :], old.astype(BF16))
            product = product.astype(BF16)
            placed = jnp.concatenate([product] * GROUP, axis=0) * place_mat[...]
            att[:, columns] = cross(back_mat[...], placed).astype(BF16)
            return carry

        lax.fori_loop(0, KVH, one, 0)

    locals_[2].wait()
    locals_[3].wait()

    kv_wait_recv(0)
    if sp > 2:
        kv_start(1)

    w_wait(0, dev_x, bottom)
    w_forward(5, dev_x, bottom, dev_y)
    w_wait(2, dev_y, top)
    w_forward(4, dev_y, top, dev_x)
    w_forward(7, dev_x, bottom, mate)
    w_forward(9, dev_y, top, mate)

    attend(0)
    for step in range(1, sp - 1):
        kv_wait_recv(step)
        if step < sp - 2:
            kv_start(step + 1)
    w_wait(1, dev_x, top)
    w_forward(8, dev_x, top, mate)
    w_wait(3, dev_y, bottom)
    w_forward(10, dev_y, bottom, mate)
    for turn in range(1, pairs):
        attend(turn)

    columns_each = w_ref.shape[1]

    def project(shard, squares):
        columns = pl.ds(pl.multiple_of(shard * columns_each, columns_each), columns_each)
        result = dot(att[...], w_all[shard])
        proj[:, columns] = result
        return squares + jnp.sum(result * result, axis=1, keepdims=True)

    mate_x, mate_y, mate_d = mate + flip_x, mate + flip_y, mate + flip_x + flip_y
    locals_[4].wait()
    squares = project(here, jnp.zeros((tokens, 1), F32))
    w_wait(6, mate, whole)
    squares = project(mate, squares)
    squares = project(dev_x, squares)
    squares = project(dev_y, squares)
    w_wait(7, mate_x, bottom)
    w_wait(8, mate_x, top)
    squares = project(mate_x, squares)
    w_wait(9, mate_y, top)
    w_wait(10, mate_y, bottom)
    squares = project(mate_y, squares)
    w_wait(4, dev_d, top)
    w_forward(11, dev_d, top, mate)
    w_wait(5, dev_d, bottom)
    w_forward(12, dev_d, bottom, mate)
    squares = project(dev_d, squares)
    w_wait(11, mate_d, top)
    w_wait(12, mate_d, bottom)
    squares = project(mate_d, squares)

    inverse = lax.rsqrt(squares * (1.0 / (columns_each * dp)) + EPSILON)
    for j in range(dp):
        columns = slice(j * columns_each, (j + 1) * columns_each)
        out_ref[:, columns] = (proj[:, columns] * inverse * og_ref[:, columns]).astype(BF16)

    for copy in sent:
        copy.wait_send()
    for step in range(sp - 1):
        for way in (0, 1):
            @pl.when(kv_sends(way, step))
            def _(way=way, step=step):
                for copy in kv_copies(way, step):
                    copy.wait_send()


def per_device_fused(sp, dp, queries, keys, values, query_gain, key_gain, out_weight, out_gain):
    tokens = queries.shape[1]
    depth, columns = out_weight.shape
    hidden = queries.shape[2]
    kv_width = keys.shape[2]
    seq_len = tokens * sp
    hbm_spec = pl.BlockSpec(memory_space=pltpu.HBM)
    vmem_spec = pl.BlockSpec(memory_space=pltpu.VMEM)
    result = pl.pallas_call(
        functools.partial(kernel, sp, dp),
        out_shape=jax.ShapeDtypeStruct((tokens, columns * dp), BF16),
        in_specs=[hbm_spec] * 3 + [vmem_spec] * 2 + [hbm_spec, vmem_spec, hbm_spec],
        out_specs=vmem_spec,
        scratch_shapes=[
            pltpu.VMEM((tokens, hidden), BF16),
            pltpu.VMEM((tokens, hidden), BF16),
            pltpu.VMEM((seq_len, kv_width), BF16),
            pltpu.VMEM((seq_len, kv_width), BF16),
            pltpu.VMEM((2 * tokens, kv_width), BF16),
            pltpu.VMEM((2, seq_len, 2 * HEAD), F32),
            pltpu.VMEM((dp, depth, columns), BF16),
            pltpu.VMEM((4, 16, BLOCK), F32),
            pltpu.VMEM((BLOCK, BLOCK), BF16),
            pltpu.VMEM((BLOCK, BLOCK), BF16),
            pltpu.VMEM((BLOCK, GROUP * tokens), BF16),
            pltpu.VMEM((tokens, GROUP * tokens), BF16),
            pltpu.VMEM((sp // 2, kv_width, 2 * tokens), BF16),
            pltpu.VMEM((max(sp // 2 - 1, 1), KVH, 2 * tokens, GROUP * tokens), F32),
            pltpu.VMEM((max(sp // 2 - 1, 1), KVH, 1, GROUP * tokens), F32),
            pltpu.VMEM((max(sp // 2 - 1, 1), KVH, 1, GROUP * tokens), F32),
            pltpu.VMEM((tokens, hidden), BF16),
            pltpu.VMEM((tokens, columns * dp), F32),
            pltpu.SemaphoreType.DMA((5,)),
            pltpu.SemaphoreType.DMA((2, sp - 1, 2)),
            pltpu.SemaphoreType.DMA((2, sp - 1, 2)),
            pltpu.SemaphoreType.DMA((13,)),
            pltpu.SemaphoreType.DMA((13,)),
        ],
        compiler_params=pltpu.CompilerParams(
            collective_id=0, has_side_effects=True, vmem_limit_bytes=67043328
        ),
    )(
        queries[0], keys[0], values[0], query_gain[None], key_gain[None],
        out_weight, out_gain[None], jnp.asarray(position_tables(seq_len)),
    )
    return result[None]


def solution(mesh):
    sp, dp = mesh.shape["sp"], mesh.shape["dp"]
    if dp == 8 and sp >= 2 and sp % 2 == 0 and sp <= 4:
        body = functools.partial(per_device_fused, sp, dp)
    else:
        body = per_device_general
    return jax.shard_map(
        body,
        mesh=mesh,
        in_specs=(
            P("dp", "sp", None),
            P("dp", "sp", None),
            P("dp", "sp", None),
            P(),
            P(),
            P(None, "dp"),
            P(),
        ),
        out_specs=P("dp", "sp", None),
        check_vma=False,
    )
```

```python
import functools

import jax
import jax.numpy as jnp
import numpy as np
from jax import lax
from jax.experimental import pallas as pl
from jax.experimental.pallas import tpu as pltpu
from jax.sharding import PartitionSpec as P

QH = 16
KVH = 4
HEAD = 64
GRID_W = 64
GROUP = QH // KVH
HALVES = 2
BLOCK = GROUP * HEAD


EPSILON = 1e-06
ROTARY_BASE = 10000.0

F32 = jnp.float32
BF16 = jnp.bfloat16


def rotate(vectors, positions, width):
    half_width = width // 2
    frequency = ROTARY_BASE ** (-jnp.arange(0, width, 2, dtype=jnp.float32) / width)
    angles = positions.astype(jnp.float32)[:, None] * frequency[None, :]
    cosines = jnp.cos(angles)[:, None, :]
    sine_table = jnp.sin(angles)[:, None, :]
    first_half = vectors[..., :half_width]
    second_half = vectors[..., half_width:]
    return jnp.concatenate(
        [
            first_half * cosines - second_half * sine_table,
            second_half * cosines + first_half * sine_table,
        ],
        axis=-1,
    )


def prepare(vectors, gain_vector, grid_row, grid_col):
    vectors = vectors.astype(jnp.float32)
    vectors = (
        vectors
        * lax.rsqrt(jnp.mean(vectors * vectors, axis=-1, keepdims=True) + EPSILON)
        * gain_vector
    )
    half_width = HEAD // 2
    turned = jnp.concatenate(
        [
            rotate(vectors[..., :half_width], grid_row, half_width),
            rotate(vectors[..., half_width:], grid_col, half_width),
        ],
        axis=-1,
    )
    return turned.astype(jnp.bfloat16)


def softmax_rows(scores):
    row_max = jnp.max(scores, axis=-1, keepdims=True)
    exponent = jnp.exp(scores - row_max)
    return exponent / jnp.sum(exponent, axis=-1, keepdims=True)


def per_device_general(queries, keys, values, query_gain, key_gain, out_weight, out_gain):
    sp_count = lax.axis_size("sp")
    tokens_here = queries.shape[1]
    seq_len = tokens_here * sp_count
    score_scale = HEAD ** (-0.5)
    offset = lax.axis_index("sp") * tokens_here
    positions = offset + jnp.arange(tokens_here, dtype=jnp.int32)
    grid_row = positions // GRID_W
    grid_col = positions % GRID_W
    query_rot = prepare(queries[0].reshape(tokens_here, QH, HEAD), query_gain, grid_row, grid_col)
    key_rot = prepare(keys[0].reshape(tokens_here, KVH, HEAD), key_gain, grid_row, grid_col)
    value_heads = values[0].reshape(tokens_here, KVH, HEAD)
    kv_pairs = jnp.concatenate([key_rot, value_heads], axis=2)
    all_pairs = lax.all_gather(
        kv_pairs.reshape(tokens_here, KVH * 2 * HEAD), "sp", axis=0, tiled=True
    )
    all_pairs = all_pairs.reshape(seq_len, KVH, 2, HEAD)
    key_all = all_pairs[:, :, 0].transpose(1, 0, 2)
    value_all = all_pairs[:, :, 1].transpose(1, 0, 2)
    query_groups = query_rot.reshape(tokens_here, KVH, QH // KVH, HEAD).transpose(1, 0, 2, 3)

    def attend_group(operands):
        query_group, key_head, value_head = operands
        scores = (
            jnp.einsum("qgd,kd->gqk", query_group, key_head, preferred_element_type=jnp.float32)
            * score_scale
        )
        attn_weights = softmax_rows(scores).astype(jnp.bfloat16)
        return jnp.einsum(
            "gqk,kd->qgd", attn_weights, value_head, preferred_element_type=jnp.float32
        ).astype(jnp.bfloat16)

    results = lax.map(attend_group, (query_groups, key_all, value_all))
    attended = results.transpose(1, 0, 2, 3).reshape(tokens_here, QH * HEAD)
    projected = jnp.dot(
        attended,
        lax.all_gather(out_weight, "dp", axis=1, tiled=True),
        preferred_element_type=jnp.float32,
    )
    normed = (
        projected
        * lax.rsqrt(jnp.mean(projected * projected, axis=-1, keepdims=True) + EPSILON)
        * out_gain
    )
    return normed.astype(jnp.bfloat16)[None]


def position_tables(seq_len):
    width = HEAD // 2
    frequency = np.float32(ROTARY_BASE) ** (
        -np.arange(0, width, 2, dtype=np.float32) / np.float32(width)
    )
    position = np.arange(seq_len)
    parts = []
    for coordinate in (position // GRID_W, position % GRID_W):
        angles = coordinate.astype(np.float32)[:, None] * frequency[None, :]
        parts += [angles, angles]
    angles = np.concatenate(parts * 2, axis=1).astype(np.float64)
    return np.stack([np.cos(angles), np.sin(angles)]).astype(np.float32)


def dot(a, b):
    return jnp.dot(a, b, preferred_element_type=F32)


def cross(a, b):
    return lax.dot_general(a, b, (((1,), (1,)), ((), ())), preferred_element_type=F32)


def kernel(
    sp, dp,
    q_ref, k_ref, v_ref, qg_ref, kg_ref, w_ref, og_ref, table_ref,
    out_ref,
    q_raw, q_rot, k_all, v_all, tables, w_all, gains,
    swap_mat, ones_mat, place_mat, back_mat, v_turned,
    expo, peak, total, att, proj,
    local_sem, kv_send, kv_recv, w_send, w_recv,
):
    tokens = q_raw.shape[0]
    depth = w_ref.shape[0]
    half = depth // 2
    me = lax.axis_index("sp")
    here = lax.axis_index("dp")
    mate = here + 1 - 2 * (here % 2)
    flip_x = 2 - 4 * ((here // 2) % 2)
    flip_y = 4 - 8 * ((here // 4) % 2)
    dev_x = here + flip_x
    dev_y = here + flip_y
    dev_d = here + flip_x + flip_y

    barrier = pltpu.get_barrier_semaphore()
    has_left = me > 0
    has_right = me < sp - 1

    for other in (mate, dev_x, dev_y):
        pl.semaphore_signal(barrier, inc=1, device_id={"dp": other})

    @pl.when(has_left)
    def _():
        pl.semaphore_signal(barrier, inc=1, device_id={"sp": me - 1})

    @pl.when(has_right)
    def _():
        pl.semaphore_signal(barrier, inc=1, device_id={"sp": me + 1})

    locals_ = [
        pltpu.make_async_copy(q_ref, q_raw, local_sem.at[0]),
        pltpu.make_async_copy(table_ref, tables, local_sem.at[1]),
        pltpu.make_async_copy(k_ref, k_all.at[pl.ds(me * tokens, tokens)], local_sem.at[2]),
        pltpu.make_async_copy(v_ref, v_all.at[pl.ds(me * tokens, tokens)], local_sem.at[3]),
        pltpu.make_async_copy(w_ref, w_all.at[here], local_sem.at[4]),
    ]
    for copy in locals_:
        copy.start()

    pl.semaphore_wait(barrier, 3 + jnp.minimum(me, 1) + jnp.minimum(sp - 1 - me, 1))

    part = k_ref.shape[1] // HALVES

    def kv_copies(way, step, side):
        block = me - step if way == 0 else me + step
        target = me + 1 if way == 0 else me - 1
        rows = pl.ds(block * tokens, tokens)
        columns = pl.ds(side * part, part)
        copies = []
        for i, (own, every) in enumerate(((k_ref, k_all), (v_ref, v_all))):
            copies.append(
                pltpu.make_async_remote_copy(
                    src_ref=own.at[:, columns] if step == 0 else every.at[rows, columns],
                    dst_ref=every.at[rows, columns],
                    send_sem=kv_send.at[way, step, side, i],
                    recv_sem=kv_recv.at[way, step, side, i],
                    device_id={"sp": target},
                )
            )
        return copies

    def kv_sends(way, step):
        if way == 0:
            return jnp.logical_and(has_right, me - step >= 0)
        return jnp.logical_and(has_left, me + step < sp)

    def kv_start(step, side):
        if step >= sp - 1:
            return
        for way in (0, 1):
            @pl.when(kv_sends(way, step))
            def _(way=way):
                for copy in kv_copies(way, step, side):
                    copy.start()

    def kv_arrive(step, side):
        for way in (0, 1):
            source = me - 1 - step if way == 0 else me + 1 + step
            arrives = source >= 0 if way == 0 else source < sp

            @pl.when(arrives)
            def _(way=way, source=source):
                window = (pl.ds(source * tokens, tokens), pl.ds(side * part, part))
                for i, every in enumerate((k_all, v_all)):
                    pltpu.make_async_remote_copy(
                        src_ref=every.at[window],
                        dst_ref=every.at[window],
                        send_sem=kv_send.at[way, step, side, i],
                        recv_sem=kv_recv.at[way, step, side, i],
                        device_id={"sp": me},
                    ).wait_recv()
        kv_start(step + 1, side)

    for side in range(HALVES):
        kv_start(0, side)

    top, bottom, whole = (0, half), (half, half), (0, depth)

    def w_copy(index, shard, rows, target, own=False):
        window = pl.ds(rows[0], rows[1])
        return pltpu.make_async_remote_copy(
            src_ref=w_ref.at[window] if own else w_all.at[shard, window],
            dst_ref=w_all.at[shard, window],
            send_sem=w_send.at[index],
            recv_sem=w_recv.at[index],
            device_id={"dp": target},
        )

    def w_wait(index, shard, rows):
        w_copy(index, shard, rows, mate).wait_recv()

    sent = [
        w_copy(0, here, bottom, dev_x, own=True),
        w_copy(2, here, top, dev_y, own=True),
        w_copy(1, here, top, dev_x, own=True),
        w_copy(3, here, bottom, dev_y, own=True),
        w_copy(6, here, whole, mate, own=True),
    ]
    for copy in sent:
        copy.start()

    def w_forward(index, shard, rows, target):
        copy = w_copy(index, shard, rows, target)
        copy.start()
        sent.append(copy)

    row_id = lax.broadcasted_iota(jnp.int32, (BLOCK, BLOCK), 0)
    col_id = lax.broadcasted_iota(jnp.int32, (BLOCK, BLOCK), 1)
    quarter = HEAD // 4
    second = (col_id & (HEAD // 2 - 1)) >= quarter
    partner_col = jnp.where(second, col_id - quarter, col_id + quarter)
    hit = row_id == partner_col
    swap_mat[...] = jnp.where(hit, jnp.where(second, 1.0, -1.0), 0.0).astype(BF16)
    ones_mat[...] = jnp.where((row_id // HEAD) == (col_id // HEAD), 1.0, 0.0).astype(BF16)
    spread = jnp.where(
        row_id[:HEAD] == (col_id[:HEAD] & (HEAD - 1)), 1.0, 0.0
    ).astype(BF16)
    spread_swapped = jnp.where(
        row_id[:HEAD] == (partner_col[:HEAD] & (HEAD - 1)), 1.0, 0.0
    ).astype(BF16)
    for i, gain_ref in enumerate((qg_ref, kg_ref)):
        gain = jnp.broadcast_to(gain_ref[...], (16, HEAD))
        first = gain.astype(BF16)
        rest = gain - first.astype(F32)
        mid = rest.astype(BF16)
        low = (rest - mid.astype(F32)).astype(BF16)
        for j, matrix in enumerate((spread, spread_swapped)):
            gains[2 * i + j] = (dot(first, matrix) + dot(mid, matrix)) + dot(low, matrix)

    lane_head = lax.broadcasted_iota(jnp.int32, (1, BLOCK), 1) // HEAD
    masks = [jnp.where(lane_head == p, 1.0, 0.0) for p in range(GROUP)]

    def turned(x, rows, which, scale):
        xf = x.astype(F32)
        square = xf * xf
        high = square.astype(BF16)
        low = (square - high.astype(F32)).astype(BF16)
        size = x.shape[1]
        ones = ones_mat[:size, :size]
        mean = (dot(high, ones) + dot(low, ones)) * (1.0 / HEAD)
        inverse = lax.rsqrt(mean + EPSILON) * scale
        swapped = dot(x, swap_mat[:size, :size])
        cosines = tables[0, rows, :]
        sines = tables[1, rows, :]
        if size > 2 * HEAD:
            cosines = jnp.concatenate([cosines, cosines], axis=1)
            sines = jnp.concatenate([sines, sines], axis=1)
        cosines = cosines * gains[2 * which, 0:1, :size]
        sines = sines * gains[2 * which + 1, 0:1, :size]
        return ((xf * cosines + swapped * sines) * inverse).astype(BF16)

    locals_[0].wait()
    locals_[1].wait()
    own_rows = pl.ds(pl.multiple_of(me * tokens, 64), tokens)
    for b in range(KVH):
        columns = slice(b * BLOCK, (b + 1) * BLOCK)
        q_rot[:, columns] = turned(q_raw[:, columns], own_rows, 0, HEAD ** (-0.5))

    pairs = sp // 2
    mine = me // 2

    eye = jnp.where(row_id == col_id, 1.0, 0.0).astype(BF16)
    wide = GROUP * tokens
    lane = lax.broadcasted_iota(jnp.int32, (BLOCK, wide), 1)
    line = lax.broadcasted_iota(jnp.int32, (BLOCK, wide), 0) // HEAD * tokens
    inside = jnp.logical_and(lane >= line, lane < line + tokens)
    place_mat[...] = jnp.where(inside, 1.0, 0.0).astype(BF16)
    lane = lax.broadcasted_iota(jnp.int32, (tokens, wide), 1)
    line = lax.broadcasted_iota(jnp.int32, (tokens, wide), 0)
    hit = lane == line
    for p in range(1, GROUP):
        hit = jnp.logical_or(hit, lane == line + p * tokens)
    back_mat[...] = jnp.where(hit, 1.0, 0.0).astype(BF16)

    def attend(turn, side):
        span = 2 * tokens
        pair = lax.rem(mine + turn, pairs)
        rows = pl.ds(pl.multiple_of(pair * span, 128), span)
        lanes = slice(side * part, (side + 1) * part)
        key_side = turned(k_all[rows, lanes], rows, 1, 1.0)
        v_turned[turn, lanes, :] = cross(eye[:part, :part], v_all[rows, lanes]).astype(BF16)
        heads = KVH // HALVES

        def one(b):
            columns = slice(b * BLOCK, (b + 1) * BLOCK)
            value_rows = slice(b * HEAD, (b + 1) * HEAD)
            source = (b - side * heads) * HEAD + (col_id[:part] & (HEAD - 1))
            pick = jnp.where(row_id[:part] == source, 1.0, 0.0).astype(BF16)
            key = dot(key_side, pick).astype(BF16)
            query = q_rot[:, columns]
            query = jnp.concatenate([query * mask.astype(BF16) for mask in masks], axis=0)
            scores = cross(key, query)
            high = jnp.max(scores, axis=0, keepdims=True)
            if turn < pairs - 1:
                weights = jnp.exp(scores - high)
                expo[turn, b] = weights
                peak[turn, b] = high
                total[turn, b] = jnp.sum(weights, axis=0, keepdims=True)
                return
            for t in range(turn):
                high = jnp.maximum(high, peak[t, b])
            weights = jnp.exp(scores - high)
            norm = jnp.sum(weights, axis=0, keepdims=True)
            keeps = [jnp.exp(peak[t, b] - high) for t in range(turn)]
            for t in range(turn):
                norm = norm + total[t, b] * keeps[t]
            inverse = 1.0 / norm
            product = dot(v_turned[turn, value_rows, :], (weights * inverse).astype(BF16))
            for t in range(turn):
                old = expo[t, b] * (keeps[t] * inverse)
                product = product + dot(v_turned[t, value_rows, :], old.astype(BF16))
            product = product.astype(BF16)
            placed = jnp.concatenate([product] * GROUP, axis=0) * place_mat[...]
            att[:, columns] = cross(back_mat[...], placed).astype(BF16)

        for b in range(side * heads, (side + 1) * heads):
            one(b)

    locals_[2].wait()
    locals_[3].wait()

    last = HALVES - 1
    for side in range(HALVES):
        kv_arrive(0, side)
    for side in range(last):
        attend(0, side)

    w_wait(0, dev_x, bottom)
    w_forward(5, dev_x, bottom, dev_y)
    w_wait(2, dev_y, top)
    w_forward(4, dev_y, top, dev_x)
    w_forward(7, dev_x, bottom, mate)
    w_forward(9, dev_y, top, mate)
    for step in range(1, sp - 2):
        for side in range(HALVES):
            kv_arrive(step, side)

    attend(0, last)
    if sp > 2:
        for side in range(HALVES):
            kv_arrive(sp - 2, side)
            if side == last:
                w_wait(1, dev_x, top)
                w_forward(8, dev_x, top, mate)
                w_wait(3, dev_y, bottom)
                w_forward(10, dev_y, bottom, mate)
            for turn in range(1, pairs):
                attend(turn, side)
    else:
        w_wait(1, dev_x, top)
        w_forward(8, dev_x, top, mate)
        w_wait(3, dev_y, bottom)
        w_forward(10, dev_y, bottom, mate)

    columns_each = w_ref.shape[1]

    def project(shard, squares):
        columns = pl.ds(pl.multiple_of(shard * columns_each, columns_each), columns_each)
        result = dot(att[...], w_all[shard])
        proj[:, columns] = result
        return squares + jnp.sum(result * result, axis=1, keepdims=True)

    mate_x, mate_y, mate_d = mate + flip_x, mate + flip_y, mate + flip_x + flip_y
    locals_[4].wait()
    squares = project(here, jnp.zeros((tokens, 1), F32))
    w_wait(6, mate, whole)
    squares = project(mate, squares)
    squares = project(dev_x, squares)
    squares = project(dev_y, squares)
    w_wait(7, mate_x, bottom)
    w_wait(8, mate_x, top)
    squares = project(mate_x, squares)
    w_wait(9, mate_y, top)
    w_wait(10, mate_y, bottom)
    squares = project(mate_y, squares)
    w_wait(4, dev_d, top)
    w_forward(11, dev_d, top, mate)
    w_wait(5, dev_d, bottom)
    w_forward(12, dev_d, bottom, mate)
    squares = project(dev_d, squares)
    w_wait(11, mate_d, top)
    w_wait(12, mate_d, bottom)
    squares = project(mate_d, squares)

    inverse = lax.rsqrt(squares * (1.0 / (columns_each * dp)) + EPSILON)
    for j in range(dp):
        columns = slice(j * columns_each, (j + 1) * columns_each)
        out_ref[:, columns] = (proj[:, columns] * inverse * og_ref[:, columns]).astype(BF16)

    for copy in sent:
        copy.wait_send()
    for step in range(sp - 1):
        for way in (0, 1):
            @pl.when(kv_sends(way, step))
            def _(way=way, step=step):
                for side in range(HALVES):
                    for copy in kv_copies(way, step, side):
                        copy.wait_send()


def per_device_fused(sp, dp, queries, keys, values, query_gain, key_gain, out_weight, out_gain):
    tokens = queries.shape[1]
    depth, columns = out_weight.shape
    hidden = queries.shape[2]
    kv_width = keys.shape[2]
    seq_len = tokens * sp
    hbm_spec = pl.BlockSpec(memory_space=pltpu.HBM)
    vmem_spec = pl.BlockSpec(memory_space=pltpu.VMEM)
    result = pl.pallas_call(
        functools.partial(kernel, sp, dp),
        out_shape=pltpu.VMEM((tokens, columns * dp), BF16),
        in_specs=[hbm_spec] * 3 + [vmem_spec] * 2 + [hbm_spec, vmem_spec, hbm_spec],
        out_specs=vmem_spec,
        scratch_shapes=[
            pltpu.VMEM((tokens, hidden), BF16),
            pltpu.VMEM((tokens, hidden), BF16),
            pltpu.VMEM((seq_len, kv_width), BF16),
            pltpu.VMEM((seq_len, kv_width), BF16),
            pltpu.VMEM((2, seq_len, 2 * HEAD), F32),
            pltpu.VMEM((dp, depth, columns), BF16),
            pltpu.VMEM((4, 16, BLOCK), F32),
            pltpu.VMEM((BLOCK, BLOCK), BF16),
            pltpu.VMEM((BLOCK, BLOCK), BF16),
            pltpu.VMEM((BLOCK, GROUP * tokens), BF16),
            pltpu.VMEM((tokens, GROUP * tokens), BF16),
            pltpu.VMEM((sp // 2, kv_width, 2 * tokens), BF16),
            pltpu.VMEM((max(sp // 2 - 1, 1), KVH, 2 * tokens, GROUP * tokens), F32),
            pltpu.VMEM((max(sp // 2 - 1, 1), KVH, 1, GROUP * tokens), F32),
            pltpu.VMEM((max(sp // 2 - 1, 1), KVH, 1, GROUP * tokens), F32),
            pltpu.VMEM((tokens, hidden), BF16),
            pltpu.VMEM((tokens, columns * dp), F32),
            pltpu.SemaphoreType.DMA((5,)),
            pltpu.SemaphoreType.DMA((2, sp - 1, HALVES, 2)),
            pltpu.SemaphoreType.DMA((2, sp - 1, HALVES, 2)),
            pltpu.SemaphoreType.DMA((13,)),
            pltpu.SemaphoreType.DMA((13,)),
        ],
        compiler_params=pltpu.CompilerParams(
            collective_id=0, has_side_effects=True, vmem_limit_bytes=66000000
        ),
    )(
        queries[0], keys[0], values[0], query_gain[None], key_gain[None],
        out_weight, out_gain[None], jnp.asarray(position_tables(seq_len)),
    )
    return result[None]


def solution(mesh):
    sp, dp = mesh.shape["sp"], mesh.shape["dp"]
    if dp == 8 and sp >= 2 and sp % 2 == 0 and sp <= 4:
        body = functools.partial(per_device_fused, sp, dp)
    else:
        body = per_device_general
    return jax.shard_map(
        body,
        mesh=mesh,
        in_specs=(
            P("dp", "sp", None),
            P("dp", "sp", None),
            P("dp", "sp", None),
            P(),
            P(),
            P(None, "dp"),
            P(),
        ),
        out_specs=P("dp", "sp", None),
        check_vma=False,
    )
```
